32 devices in a mesh: ep: 16 (over z, y, x), tp: 2 (over core).
Axes of the slice: x: 2, y: 2, z: 4, core: 2. Of those that a mesh axis runs over, the one named last changes fastest.
Arguments:
- tokens_in: bfloat16 [512, 2048], P('ep'), may hold values from -6 to 6
- state_in: float32 [512, 8, 64, 64], P('ep', 'tp'), may hold values from -4 to 4
- norm_mix: bfloat16 [2048], replicated, may hold values from 0.099609375 to 1.8984375
- w_recept: bfloat16 [2048, 512], P(None, 'tp'), may hold values from -0.125 to 0.125
- w_key: bfloat16 [2048, 512], P(None, 'tp'), may hold values from -0.125 to 0.125
- w_value: bfloat16 [2048, 512], P(None, 'tp'), may hold values from -0.125 to 0.125
- decay_down: bfloat16 [2048, 64], replicated, may hold values from -0.125 to 0.125
- decay_up: bfloat16 [64, 512], P(None, 'tp'), may hold values from -0.75 to 0.75
- decay_base: float32 [512], P('tp'), may hold values from -4 to 2
- iclr_down: bfloat16 [2048, 64], replicated, may hold values from -0.125 to 0.125
- iclr_up: bfloat16 [64, 512], P(None, 'tp'), may hold values from -0.75 to 0.75
- iclr_base: float32 [512], P('tp'), may hold values from -4 to 4
- key_scale: bfloat16 [512], P('tp'), may hold values from 0.099609375 to 1.8984375
- key_mix: bfloat16 [512], P('tp'), may hold values from 0.099609375 to 1.8984375
- w_out: bfloat16 [512, 2048], P('tp'), may hold values from -0.046875 to 0.046875
- norm_moe: bfloat16 [2048], replicated, may hold values from 0.099609375 to 1.8984375
- router_group: bfloat16 [2048, 2], replicated, may hold values from -0.125 to 0.125
- router_expert: bfloat16 [2048, 16], replicated, may hold values from -0.125 to 0.125
- routes: int32 [512, 4], P('ep'), may hold values from 0 to 15, as said below
- expert_gate: bfloat16 [16, 2048, 256], P('ep', None, 'tp'), may hold values from -0.125 to 0.125
- expert_up: bfloat16 [16, 2048, 256], P('ep', None, 'tp'), may hold values from -0.125 to 0.125
- expert_down: bfloat16 [16, 256, 2048], P('ep', 'tp'), may hold values from -1.5 to 1.5
Outputs:
- layer_out: bfloat16 [512, 2048], P('ep', 'tp')
- state_out: float32 [512, 8, 64, 64], P('ep', 'tp')
The draws below stay inside these ranges and needn't reach their ends.
Inputs may be any that keep to these rules, and one draw needn't show every extreme that they name: `routes`: each row names 4 different experts of one group (the same value of id // 8). Among the rows of one device no expert is named by more than 16 rows, and in every draw one expert is named by exactly 16 rows of every device.
All inputs are finite; a program needn't handle non-finite values.
Results may differ from the reference program's by a relative error of at most 0.018.
Values may be sent and summed in bfloat16 or wider, within the bound.
A program may use at most 64 MiB of HBM per device.

```python
import jax
import jax.numpy as jnp
from jax import lax

D = 2048
HEADS = 8
HEAD = 64
RANK = 64
FE = 256
GROUP_EXPERTS = 8
TOPK = 4
SEQ_DEV = 32
WIDTH = 512
TOKENS = 512
EXPERTS = 16
GROUPS = 2
CAP = 16
N_EP = 16
N_TP = 2


def draw_routes(key, part):
    base = jax.random.fold_in(key, 7)
    keys = jax.random.split(base, 7)
    blocks = TOKENS // SEQ_DEV
    total_rows = blocks * SEQ_DEV
    hot_group = jax.random.randint(keys[0], (), 0, GROUPS)
    hot_inner = jax.random.randint(keys[1], (), 0, GROUP_EXPERTS)
    order = jax.vmap(lambda sub: jax.random.permutation(sub, SEQ_DEV))(jax.random.split(keys[2], blocks))
    band = order // CAP
    others = jax.vmap(lambda sub: jax.random.permutation(sub, max(GROUPS - 1, 1)))(jax.random.split(keys[3], blocks))
    chosen = jnp.take_along_axis(others, jnp.maximum(band - 1, 0), axis=1)
    group_ids = jnp.where(band == 0, hot_group, (hot_group + 1 + chosen) % GROUPS).reshape(total_rows, 1)
    free_pick = jax.vmap(lambda sub: jax.random.permutation(sub, GROUP_EXPERTS))(jax.random.split(keys[4], total_rows))[:, :TOPK]
    rest = jax.vmap(lambda sub: jax.random.permutation(sub, GROUP_EXPERTS - 1))(jax.random.split(keys[5], total_rows))[:, :TOPK - 1]
    forced = jnp.concatenate([jnp.zeros((total_rows, 1), jnp.int32) + hot_inner, (hot_inner + 1 + rest) % GROUP_EXPERTS], axis=1)
    inner = jnp.where(band.reshape(total_rows, 1) == 0, forced, free_pick)
    column_order = jax.vmap(lambda sub: jax.random.permutation(sub, TOPK))(jax.random.split(keys[6], total_rows))
    inner = jnp.take_along_axis(inner, column_order, axis=1)
    return (group_ids * GROUP_EXPERTS + inner).astype(jnp.int32)


def steps_of(rng, extent, pieces, least, high):
    gain = 1.0
    for dim, parts in pieces:
        draws = jax.random.uniform(jax.random.fold_in(jax.random.fold_in(rng, 6), dim), (parts,), jnp.float32, least / len(pieces), high / len(pieces))
        gain = gain * jnp.repeat(jnp.exp(draws), extent[dim] // parts).reshape((-1,) + (1,) * (len(extent) - 1 - dim))
    return gain


def centred(own_key, shape, scale, reach, shards=(), held_as=jnp.bfloat16):
    values = jax.random.normal(own_key, shape, jnp.float32) * scale
    if len(shards) > 0:
        values = steps_of(own_key, shape, shards, -0.22, 0.18) * values
    return jnp.clip(values, min=-reach, max=reach).astype(held_as)


def setup_inputs(seed: int = 0) -> dict:
    streams_of = jax.random.split(jax.random.key(seed), 23)
    return {
        "tokens_in": centred(streams_of[0], (TOKENS, D), 1.0, 6.0, ((0, 16),)),
        "state_in": centred(streams_of[1], (TOKENS, HEADS, HEAD, HEAD), 0.5, 4.0, ((0, 16), (1, 2)), jnp.float32),
        "norm_mix": jnp.clip(1.0 + 0.18 * jax.random.normal(streams_of[2], (D,), jnp.float32), 0.099609375, 1.8984375).astype(jnp.bfloat16),
        "w_recept": centred(streams_of[3], (D, WIDTH), D ** -0.5, 0.125, ((1, 2),)),
        "w_key": centred(streams_of[4], (D, WIDTH), D ** -0.5, 0.125, ((1, 2),)),
        "w_value": centred(streams_of[5], (D, WIDTH), D ** -0.5, 0.125, ((1, 2),)),
        "decay_down": centred(streams_of[6], (D, RANK), D ** -0.5, 0.125),
        "decay_up": centred(streams_of[7], (RANK, WIDTH), RANK ** -0.5, 0.75, ((1, 2),)),
        "decay_base": jnp.clip(-4.0 + 6.0 * jax.random.uniform(streams_of[8], (WIDTH,), jnp.float32) ** steps_of(streams_of[8], (WIDTH,), ((0, 2),), -0.2, 0.2), -4.0, 2.0),
        "iclr_down": centred(streams_of[9], (D, RANK), D ** -0.5, 0.125),
        "iclr_up": centred(streams_of[10], (RANK, WIDTH), RANK ** -0.5, 0.75, ((1, 2),)),
        "iclr_base": centred(streams_of[11], (WIDTH,), 1.0, 4.0, ((0, 2),), jnp.float32),
        "key_scale": jnp.clip(1.0 + 0.18 * jax.random.normal(streams_of[12], (WIDTH,), jnp.float32), 0.099609375, 1.8984375).astype(jnp.bfloat16),
        "key_mix": jnp.clip(1.0 + 0.18 * jax.random.normal(streams_of[13], (WIDTH,), jnp.float32), 0.099609375, 1.8984375).astype(jnp.bfloat16),
        "w_out": centred(streams_of[14], (WIDTH, D), (32 * WIDTH) ** -0.5, 0.046875, ((0, 2),)),
        "norm_moe": jnp.clip(1.0 + 0.18 * jax.random.normal(streams_of[15], (D,), jnp.float32), 0.099609375, 1.8984375).astype(jnp.bfloat16),
        "router_group": centred(streams_of[16], (D, GROUPS), D ** -0.5, 0.125),
        "router_expert": centred(streams_of[17], (D, EXPERTS), D ** -0.5, 0.125),
        "routes": draw_routes(jax.random.fold_in(streams_of[22], 71), 0),
        "expert_gate": centred(streams_of[19], (EXPERTS, D, FE), D ** -0.5, 0.125, ((0, 16), (2, 2))),
        "expert_up": centred(streams_of[20], (EXPERTS, D, FE), D ** -0.5, 0.125, ((0, 16), (2, 2))),
        "expert_down": centred(streams_of[21], (EXPERTS, FE, D), (FE // 16) ** -0.5, 1.5, ((0, 16), (1, 2))),
    }


def rms_scale(values, weights):
    values32 = values.astype(jnp.float32)
    factor = lax.rsqrt(lax.optimization_barrier(jnp.mean(values32 * values32, axis=-1, keepdims=True)) + 1e-06)
    return (values32 * factor * weights.astype(jnp.float32)).astype(jnp.bfloat16)

def split_heads(values):
    return values.astype(jnp.float32).reshape(values.shape[0], HEADS, HEAD)

def expert_rows(moe_rows, gate_weight, up_weight, down_weight):
    gate_part = jnp.dot(moe_rows, gate_weight, preferred_element_type=jnp.float32)
    up_part = jnp.dot(moe_rows, up_weight, preferred_element_type=jnp.float32)
    hidden = (jax.nn.silu(gate_part) * up_part).astype(jnp.bfloat16)
    block = FE // N_TP
    total = jnp.zeros((moe_rows.shape[0], D), jnp.float32)
    for index in range(N_TP):
        partial_value = jnp.dot(hidden[:, index * block:(index + 1) * block], down_weight[index * block:(index + 1) * block], preferred_element_type=jnp.float32).astype(jnp.bfloat16)
        partial_value = lax.optimization_barrier(partial_value)
        total = total + partial_value.astype(jnp.float32)
    return total.astype(jnp.bfloat16)

def reference(tokens_in, state_in, norm_mix, w_recept, w_key, w_value, decay_down, decay_up, decay_base, iclr_down, iclr_up, iclr_base, key_scale, key_mix, w_out, norm_moe, router_group, router_expert, routes, expert_gate, expert_up, expert_down):
    f32 = jnp.float32
    bf16 = jnp.bfloat16
    normed = rms_scale(tokens_in, norm_mix)
    recept = jnp.dot(normed, w_recept, preferred_element_type=f32).astype(bf16)
    key_rows = jnp.dot(normed, w_key, preferred_element_type=f32).astype(bf16)
    value_rows = jnp.dot(normed, w_value, preferred_element_type=f32).astype(bf16)
    decay_low = jnp.tanh(jnp.dot(normed, decay_down, preferred_element_type=f32)).astype(bf16)
    iclr_low = jnp.dot(normed, iclr_down, preferred_element_type=f32).astype(bf16)
    log_rate = -jax.nn.softplus(-(decay_base.astype(f32) + jnp.dot(decay_low, decay_up, preferred_element_type=f32))) - 0.5
    decays = jnp.exp(-jnp.exp(log_rate))
    learn_rate = jax.nn.sigmoid(iclr_base.astype(f32) + jnp.dot(iclr_low, iclr_up, preferred_element_type=f32))
    recept_heads = split_heads(recept)
    key_heads = split_heads(key_rows)
    value_heads = split_heads(value_rows)
    rate_heads = split_heads(learn_rate)
    decay_heads = split_heads(decays)
    scaled = key_heads * key_scale.astype(f32).reshape(HEADS, HEAD)
    unit_key = scaled * lax.rsqrt(lax.optimization_barrier(jnp.sum(scaled * scaled, axis=-1, keepdims=True)) + 1e-06)
    key_mod = key_heads * (1.0 + (rate_heads - 1.0) * key_mix.astype(f32).reshape(HEADS, HEAD))
    removed = jnp.einsum('shvk,shk->shv', state_in, unit_key)
    state_out = state_in * decay_heads[:, :, None, :] - removed[..., None] * (unit_key * rate_heads)[:, :, None, :] + value_heads[..., None] * key_mod[:, :, None, :]
    mixed = jnp.einsum('shvk,shk->shv', state_out, recept_heads).reshape(TOKENS, WIDTH).astype(bf16)
    mixer_out = jnp.dot(mixed, w_out, preferred_element_type=f32).astype(bf16)
    x_mid = (tokens_in.astype(f32) + mixer_out.astype(f32)).astype(bf16)
    moe_in = rms_scale(x_mid, norm_moe)
    group_id = routes[:, 0] // GROUP_EXPERTS
    group_logit = jnp.dot(moe_in, router_group, preferred_element_type=f32)
    group_hit = group_id[:, None] == jnp.arange(GROUPS, dtype=jnp.int32)[None, :]
    group_prob = jax.nn.sigmoid(lax.optimization_barrier(jnp.sum(jnp.where(group_hit, group_logit, 0.0), axis=1)))
    expert_logit = jnp.dot(moe_in, router_expert, preferred_element_type=f32)
    expert_hit = routes[:, :, None] == jnp.arange(EXPERTS, dtype=jnp.int32)[None, None, :]
    scores = jax.nn.sigmoid(lax.optimization_barrier(jnp.sum(jnp.where(expert_hit, expert_logit[:, None, :], 0.0), axis=2)))
    route_weight = group_prob[:, None] * scores / lax.optimization_barrier(jnp.sum(scores, axis=1, keepdims=True))
    limit = N_EP * CAP

    def visit(total, inputs):
        gate_weight, up_weight, down_weight, expert_index = inputs
        used = jnp.any(routes == expert_index, axis=1)
        found = jnp.nonzero(used, size=limit, fill_value=TOKENS)[0].astype(jnp.int32)
        valid = (found < TOKENS).astype(f32)
        safe = jnp.minimum(found, TOKENS - 1).astype(jnp.int32)
        results = expert_rows(moe_in[safe], gate_weight, up_weight, down_weight)
        weight = lax.optimization_barrier(jnp.sum(jnp.where(routes[safe] == expert_index, route_weight[safe], 0.0), axis=1)) * valid
        return (total.at[safe].add(weight[:, None] * results.astype(f32)), None)
    total, unused = lax.scan(visit, jnp.zeros((TOKENS, D), f32), (expert_gate, expert_up, expert_down, jnp.arange(EXPERTS, dtype=jnp.int32)))
    layer_out = (x_mid.astype(f32) + total).astype(bf16)
    return (layer_out, state_out)
```

```python
import functools

import jax
import jax.numpy as jnp
from jax import lax
from jax.experimental import pallas as pl
from jax.experimental.pallas import tpu as pltpu
from jax.sharding import PartitionSpec as P


def rms_scale(values, weights):
    values32 = values.astype(jnp.float32)
    factor = lax.rsqrt(jnp.mean(values32 * values32, axis=-1, keepdims=True) + 1e-06)
    return (values32 * factor * weights.astype(jnp.float32)).astype(jnp.bfloat16)


def moe_kernel(
    ep_count,
    block_rows,
    mixed_ref,
    w_out_ref,
    tokens_ref,
    norm_ref,
    router_group_ref,
    router_expert_ref,
    group_hit_ref,
    uses_ref,
    placement_ref,
    chooser_ref,
    gate_ref,
    up_ref,
    down_ref,
    out_ref,
    part_buf,
    part_recv,
    mid_buf,
    norm_buf,
    send_buf,
    rows_buf,
    hidden_buf,
    term_send,
    term_own,
    term_recv,
    result_buf,
    back_buf,
    part_sems,
    out_send_sems,
    out_recv_sems,
    pair_send_sems,
    pair_recv_sems,
    term_send_sems,
    term_recv_sems,
    back_send_sems,
    back_recv_sems,
):
    f32 = jnp.float32
    bf16 = jnp.bfloat16
    me = lax.axis_index("ep")
    core = lax.axis_index("tp")
    other = 1 - core
    seq_count, width = tokens_ref.shape
    half = width // 2
    cap = send_buf.shape[1]
    total_rows = ep_count * cap
    per_block = block_rows // cap
    n_blocks = total_rows // block_rows
    mesh_ids = pl.DeviceIdType.MESH

    def peer_at(step):
        return lax.rem(me + step, ep_count)

    def step_at(index):
        return 1 + lax.rem(index + ep_count // 2 - 1, ep_count - 1)

    barrier = pltpu.get_barrier_semaphore()
    pl.semaphore_signal(barrier, inc=1, device_id=(me, other), device_id_type=mesh_ids)

    def greet(step, carry):
        pl.semaphore_signal(
            barrier, inc=1, device_id=(peer_at(step), core), device_id_type=mesh_ids
        )
        return carry

    lax.fori_loop(1, ep_count, greet, 0)

    for index in range(2):
        columns = slice(index * half, (index + 1) * half)
        part_buf[index] = jnp.dot(
            mixed_ref[...], w_out_ref[:, columns], preferred_element_type=f32
        )
    pl.semaphore_wait(barrier, ep_count)

    def pair_copy(source, target, send_sem, recv_sem):
        return pltpu.make_async_remote_copy(
            src_ref=source,
            dst_ref=target,
            send_sem=send_sem,
            recv_sem=recv_sem,
            device_id=(me, other),
            device_id_type=mesh_ids,
        )

    part_copy = pair_copy(part_buf, part_recv, part_sems.at[0], part_sems.at[1])
    part_copy.start()
    part_copy.wait()

    squares = jnp.zeros((seq_count, 1), f32)
    for index in range(2):
        columns = slice(index * half, (index + 1) * half)
        mixer_out = (part_buf[index] + part_recv[index]).astype(bf16)
        mid = (tokens_ref[:, columns].astype(f32) + mixer_out.astype(f32)).astype(bf16)
        mid_buf[index] = mid
        mid32 = mid.astype(f32)
        squares = squares + jnp.sum(mid32 * mid32, axis=1, keepdims=True)
    factor = lax.rsqrt(squares / width + 1e-06)
    for index in range(2):
        columns = slice(index * half, (index + 1) * half)
        norm_buf[index] = (
            mid_buf[index].astype(f32) * factor * norm_ref[:, columns].astype(f32)
        ).astype(bf16)

    own_norm = norm_buf[core]
    for index in range(n_blocks):
        rows = jnp.dot(
            placement_ref[index * block_rows : (index + 1) * block_rows, :],
            own_norm,
            preferred_element_type=f32,
        ).astype(bf16)
        send_buf[index * per_block : (index + 1) * per_block] = rows.reshape(per_block, cap, half)

    def out_copy(step):
        peer = peer_at(step)
        return pltpu.make_async_remote_copy(
            src_ref=send_buf.at[peer],
            dst_ref=rows_buf.at[core, me],
            send_sem=out_send_sems.at[step],
            recv_sem=out_recv_sems.at[step],
            device_id=(peer, core),
            device_id_type=mesh_ids,
        )

    def rows_copy(step):
        source = lax.rem(me + ep_count - step, ep_count)
        return pair_copy(
            rows_buf.at[core, source],
            rows_buf.at[core, source],
            pair_send_sems.at[step],
            pair_recv_sems.at[step],
        )

    def rows_arrival(step):
        source = lax.rem(me + ep_count - step, ep_count)
        return pair_copy(
            rows_buf.at[other, source],
            rows_buf.at[other, source],
            pair_send_sems.at[step],
            pair_recv_sems.at[step],
        )

    def start_out(index, carry):
        out_copy(step_at(index)).start()
        return carry

    lax.fori_loop(0, ep_count - 1, start_out, 0)
    rows_buf[core, me] = send_buf[me]
    rows_copy(0).start()

    group_logit = jnp.zeros(group_hit_ref.shape, f32)
    expert_logit = jnp.zeros(uses_ref.shape, f32)
    for index in range(2):
        columns = slice(index * half, (index + 1) * half)
        group_logit += jnp.dot(
            norm_buf[index], router_group_ref[columns, :], preferred_element_type=f32
        )
        expert_logit += jnp.dot(
            norm_buf[index], router_expert_ref[columns, :], preferred_element_type=f32
        )
    group_prob = jax.nn.sigmoid(jnp.sum(group_logit * group_hit_ref[...], axis=1, keepdims=True))
    scores = jax.nn.sigmoid(expert_logit) * uses_ref[...]
    weights = group_prob * scores / jnp.sum(scores, axis=1, keepdims=True)
    weights_high = weights.astype(bf16)
    weights_low = (weights - weights_high.astype(f32)).astype(bf16)
    slot_expert = lax.broadcasted_iota(jnp.int32, (ep_count, total_rows), 1) // cap
    expert_ids = lax.broadcasted_iota(jnp.int32, (ep_count, total_rows), 0)
    spread = jnp.where(slot_expert == expert_ids, 1.0, 0.0).astype(bf16)
    chooser = chooser_ref[...].astype(f32)
    combine_high = (jnp.dot(weights_high, spread, preferred_element_type=f32) * chooser).astype(bf16)
    combine_low = (jnp.dot(weights_low, spread, preferred_element_type=f32) * chooser).astype(bf16)

    def relay(index, carry):
        step = step_at(ep_count - 2 - index)
        out_copy(step).wait_recv()
        rows_copy(step).start()
        return carry

    lax.fori_loop(0, ep_count - 1, relay, 0)

    def arrive(step, carry):
        rows_arrival(step).wait_recv()
        return carry

    lax.fori_loop(0, ep_count, arrive, 0)

    for index in range(n_blocks):
        experts = slice(index * per_block, (index + 1) * per_block)
        gate_part = jnp.zeros((block_rows, gate_ref.shape[1]), f32)
        up_part = jnp.zeros((block_rows, gate_ref.shape[1]), f32)
        for piece in range(2):
            columns = slice(piece * half, (piece + 1) * half)
            rows = rows_buf[piece, experts].reshape(block_rows, half)
            gate_part += jnp.dot(rows, gate_ref[columns, :], preferred_element_type=f32)
            up_part += jnp.dot(rows, up_ref[columns, :], preferred_element_type=f32)
        hidden = (gate_part / (1.0 + jnp.exp(-gate_part)) * up_part).astype(bf16)
        hidden_buf[experts] = hidden.reshape(per_block, cap, gate_ref.shape[1])

    n_parts = term_send.shape[0]
    per_part = ep_count // n_parts
    first_part = me // per_part

    def part_at(index):
        return lax.rem(first_part + index + n_parts // 2, n_parts)

    def term_copy(part):
        return pair_copy(
            term_send.at[part],
            term_recv.at[part],
            term_send_sems.at[part],
            term_recv_sems.at[part],
        )

    def part_term(part, which):
        hidden = hidden_buf[pl.ds(part * per_part, per_part)]
        hidden = hidden.reshape(per_part * cap, gate_ref.shape[1])
        term = jnp.dot(hidden, down_ref[which], preferred_element_type=f32)
        return term.astype(bf16).reshape(per_part, cap, half)

    def back_copy(peer):
        return pltpu.make_async_remote_copy(
            src_ref=result_buf.at[peer],
            dst_ref=back_buf.at[me],
            send_sem=back_send_sems.at[peer],
            recv_sem=back_recv_sems.at[me],
            device_id=(peer, core),
            device_id_type=mesh_ids,
        )

    def back_arrival(peer):
        return pltpu.make_async_remote_copy(
            src_ref=result_buf.at[peer],
            dst_ref=back_buf.at[peer],
            send_sem=back_send_sems.at[peer],
            recv_sem=back_recv_sems.at[peer],
            device_id=(peer, core),
            device_id_type=mesh_ids,
        )

    def send_terms(index, carry):
        part = part_at(index)
        term_send[part] = part_term(part, other)
        term_copy(part).start()
        return carry

    lax.fori_loop(0, n_parts, send_terms, 0)

    def own_terms(index, carry):
        part = part_at(index)
        term_own[part] = part_term(part, core)
        return carry

    lax.fori_loop(0, n_parts, own_terms, 0)

    def finish_part(index, carry):
        part = part_at(index)
        term_copy(part).wait_recv()
        total = term_own[part].astype(f32) + term_recv[part].astype(f32)
        result_buf[pl.ds(part * per_part, per_part)] = total.astype(bf16)

        def start_back(inner, carry_inner):
            peer = part * per_part + inner

            @pl.when(peer != me)
            def _():
                back_copy(peer).start()

            return carry_inner

        lax.fori_loop(0, per_part, start_back, 0)
        return carry

    lax.fori_loop(0, n_parts, finish_part, 0)
    back_buf[me] = result_buf[me]

    def finish_sends(step, carry):
        out_copy(step).wait_send()
        back_arrival(peer_at(step)).wait_recv()
        back_copy(peer_at(step)).wait_send()
        return carry

    lax.fori_loop(1, ep_count, finish_sends, 0)

    def finish_pair(step, carry):
        rows_copy(step).wait_send()
        return carry

    lax.fori_loop(0, ep_count, finish_pair, 0)

    def finish_terms(part, carry):
        term_copy(part).wait_send()
        return carry

    lax.fori_loop(0, n_parts, finish_terms, 0)

    back = back_buf[...].reshape(total_rows, half)
    moe_out = jnp.dot(combine_high, back, preferred_element_type=f32)
    moe_out += jnp.dot(combine_low, back, preferred_element_type=f32)
    out_ref[...] = (mid_buf[core].astype(f32) + moe_out).astype(bf16)


def shards(
    tokens_in,
    state_in,
    norm_mix,
    w_recept,
    w_key,
    w_value,
    decay_down,
    decay_up,
    decay_base,
    iclr_down,
    iclr_up,
    iclr_base,
    key_scale,
    key_mix,
    w_out,
    norm_moe,
    router_group,
    router_expert,
    routes,
    expert_gate,
    expert_up,
    expert_down,
):
    f32 = jnp.float32
    bf16 = jnp.bfloat16
    seq_count = tokens_in.shape[0]
    width_model = tokens_in.shape[1]
    heads_here = state_in.shape[1]
    head_size = state_in.shape[-1]
    tp_count = lax.axis_size("tp")
    ep_count = lax.axis_size("ep")

    def split_heads(values):
        return values.astype(f32).reshape(values.shape[0], heads_here, head_size)

    normed = rms_scale(tokens_in, norm_mix)
    recept = jnp.dot(normed, w_recept, preferred_element_type=f32).astype(bf16)
    key_rows = jnp.dot(normed, w_key, preferred_element_type=f32).astype(bf16)
    value_rows = jnp.dot(normed, w_value, preferred_element_type=f32).astype(bf16)
    decay_low = jnp.tanh(jnp.dot(normed, decay_down, preferred_element_type=f32)).astype(bf16)
    iclr_low = jnp.dot(normed, iclr_down, preferred_element_type=f32).astype(bf16)
    log_rate = (
        -jax.nn.softplus(-(decay_base + jnp.dot(decay_low, decay_up, preferred_element_type=f32)))
        - 0.5
    )
    decays = jnp.exp(-jnp.exp(log_rate))
    learn_rate = jax.nn.sigmoid(iclr_base + jnp.dot(iclr_low, iclr_up, preferred_element_type=f32))
    recept_heads = split_heads(recept)
    key_heads = split_heads(key_rows)
    value_heads = split_heads(value_rows)
    rate_heads = split_heads(learn_rate)
    decay_heads = split_heads(decays)
    scaled = key_heads * key_scale.astype(f32).reshape(heads_here, head_size)
    unit_key = scaled * lax.rsqrt(jnp.sum(scaled * scaled, axis=-1, keepdims=True) + 1e-06)
    key_mod = key_heads * (
        1.0 + (rate_heads - 1.0) * key_mix.astype(f32).reshape(heads_here, head_size)
    )
    removed = jnp.einsum("shvk,shk->shv", state_in, unit_key)
    state_out = (
        state_in * decay_heads[:, :, None, :]
        - removed[..., None] * (unit_key * rate_heads)[:, :, None, :]
        + value_heads[..., None] * key_mod[:, :, None, :]
    )
    mixed = (
        jnp.einsum("shvk,shk->shv", state_out, recept_heads)
        .reshape(seq_count, heads_here * head_size)
        .astype(bf16)
    )
    n_groups = router_group.shape[1]
    experts_all = router_expert.shape[1]
    group_size = experts_all // n_groups
    top_count = routes.shape[1]
    half_width = width_model // tp_count
    limit = max(2, 2 * seq_count * top_count // ep_count)
    cap = -(-limit // 16) * 16
    total_rows = experts_all * cap
    group_hit = (routes[:, :1] // group_size == jnp.arange(n_groups)[None, :]).astype(f32)
    uses = jnp.any(routes[:, :, None] == jnp.arange(experts_all)[None, None, :], axis=1)
    position = jnp.cumsum(uses.astype(jnp.int32), axis=0) - 1
    slots = jnp.where(uses, position, -1)
    chooser = (slots[:, :, None] == jnp.arange(cap)[None, None, :]).astype(bf16)
    chooser = chooser.reshape(seq_count, total_rows)
    block_rows = min(total_rows, 256)
    n_parts = min(4, ep_count)
    per_part = ep_count // n_parts
    hidden_width = expert_gate.shape[2]
    down = expert_down[0].reshape(hidden_width, tp_count, half_width).transpose(1, 0, 2)
    dma = pltpu.SemaphoreType.DMA
    layer_out = pl.pallas_call(
        functools.partial(moe_kernel, ep_count, block_rows),
        out_shape=jax.ShapeDtypeStruct((seq_count, half_width), bf16),
        in_specs=[pl.BlockSpec(memory_space=pltpu.VMEM)] * 13,
        out_specs=pl.BlockSpec(memory_space=pltpu.VMEM),
        scratch_shapes=[
            pltpu.VMEM((tp_count, seq_count, half_width), f32),
            pltpu.VMEM((tp_count, seq_count, half_width), f32),
            pltpu.VMEM((tp_count, seq_count, half_width), bf16),
            pltpu.VMEM((tp_count, seq_count, half_width), bf16),
            pltpu.VMEM((ep_count, cap, half_width), bf16),
            pltpu.VMEM((tp_count, ep_count, cap, half_width), bf16),
            pltpu.VMEM((ep_count, cap, hidden_width), bf16),
            pltpu.VMEM((n_parts, per_part, cap, half_width), bf16),
            pltpu.VMEM((n_parts, per_part, cap, half_width), bf16),
            pltpu.VMEM((n_parts, per_part, cap, half_width), bf16),
            pltpu.VMEM((ep_count, cap, half_width), bf16),
            pltpu.VMEM((ep_count, cap, half_width), bf16),
            dma((2,)),
            dma((ep_count,)),
            dma((ep_count,)),
            dma((ep_count,)),
            dma((ep_count,)),
            dma((n_parts,)),
            dma((n_parts,)),
            dma((ep_count,)),
            dma((ep_count,)),
        ],
        compiler_params=pltpu.CompilerParams(
            collective_id=0, has_side_effects=True, vmem_limit_bytes=60 * 1024 * 1024
        ),
    )(
        mixed,
        w_out,
        tokens_in,
        norm_moe.reshape(1, width_model),
        router_group,
        router_expert,
        group_hit,
        uses.astype(f32),
        chooser.T,
        chooser,
        expert_gate[0],
        expert_up[0],
        down,
    )
    return (layer_out, state_out)


def solution(mesh):
    in_specs = (
        P("ep", None),
        P("ep", "tp", None, None),
        P(),
        P(None, "tp"),
        P(None, "tp"),
        P(None, "tp"),
        P(),
        P(None, "tp"),
        P("tp"),
        P(),
        P(None, "tp"),
        P("tp"),
        P("tp"),
        P("tp"),
        P("tp", None),
        P(),
        P(),
        P(),
        P("ep", None),
        P("ep", None, "tp"),
        P("ep", None, "tp"),
        P("ep", "tp", None),
    )
    out_specs = (P("ep", "tp"), P("ep", "tp", None, None))
    return jax.shard_map(shards, mesh=mesh, in_specs=in_specs, out_specs=out_specs, check_vma=False)
```

```python
import functools

import jax
import jax.numpy as jnp
from jax import lax
from jax.experimental import pallas as pl
from jax.experimental.pallas import tpu as pltpu
from jax.sharding import PartitionSpec as P


def mixer_kernel(
    tokens_ref,
    norm_ref,
    w_recept_hbm,
    w_key_hbm,
    w_value_hbm,
    decay_down_ref,
    decay_up_ref,
    decay_base_ref,
    iclr_down_ref,
    iclr_up_ref,
    iclr_base_ref,
    key_scale_ref,
    key_mix_ref,
    state_hbm,
    mixed_ref,
    state_out_hbm,
    weights,
    state_buf,
    out_buf,
    vectors,
    value_t,
    mixed_t,
    weight_sems,
    in_sems,
    out_sems,
):
    f32 = jnp.float32
    bf16 = jnp.bfloat16
    seq_count, width = tokens_ref.shape
    heads, head_size = state_hbm.shape[1], state_hbm.shape[3]
    channels = heads * head_size
    n_chunks = in_sems.shape[0]
    per_chunk = seq_count // n_chunks
    rows_dims = (((1,), (1,)), ((), ()))
    weight_loads = [
        pltpu.make_async_copy(source, weights.at[index], weight_sems.at[index])
        for index, source in enumerate((w_key_hbm, w_value_hbm, w_recept_hbm))
    ]
    for load in weight_loads:
        load.start()
    state_loads = []
    state_stores = []
    for index in range(n_chunks):
        span = pl.ds(index * per_chunk, per_chunk)
        state_loads.append(
            pltpu.make_async_copy(state_hbm.at[span], state_buf.at[span], in_sems.at[index])
        )
        state_stores.append(
            pltpu.make_async_copy(out_buf.at[span], state_out_hbm.at[span], out_sems.at[index])
        )
        state_loads[index].start()

    tokens = tokens_ref[...].astype(f32)
    factor = lax.rsqrt(jnp.mean(tokens * tokens, axis=1, keepdims=True) + 1e-06)
    normed = (tokens * factor * norm_ref[...].reshape(1, width).astype(f32)).astype(bf16)
    decay_low = jnp.tanh(
        lax.dot_general(normed, decay_down_ref[...], rows_dims, preferred_element_type=f32)
    ).astype(bf16)
    iclr_low = lax.dot_general(
        normed, iclr_down_ref[...], rows_dims, preferred_element_type=f32
    ).astype(bf16)
    decay_in = decay_base_ref[...].reshape(1, channels) + jnp.dot(
        decay_low, decay_up_ref[...], preferred_element_type=f32
    )
    decays = jnp.exp(-jnp.exp(jnp.float32(-0.5)) * jax.nn.sigmoid(decay_in))
    rate = jax.nn.sigmoid(
        iclr_base_ref[...].reshape(1, channels)
        + jnp.dot(iclr_low, iclr_up_ref[...], preferred_element_type=f32)
    )
    projected = []
    for index in range(3):
        weight_loads[index].wait()
        rows = jnp.dot(normed, weights[index], preferred_element_type=f32)
        projected.append(rows.astype(bf16).astype(f32))
    key, value, recept = projected
    value_t[...] = value.T
    scaled = key * key_scale_ref[...].reshape(1, channels).astype(f32)
    key_mod = key * (1.0 + (rate - 1.0) * key_mix_ref[...].reshape(1, channels).astype(f32))
    for head in range(heads):
        span = slice(head * head_size, (head + 1) * head_size)
        part = scaled[:, span]
        unit = part * lax.rsqrt(jnp.sum(part * part, axis=1, keepdims=True) + 1e-06)
        vectors[0, head] = decays[:, span]
        vectors[1, head] = unit
        vectors[2, head] = unit * rate[:, span]
        vectors[3, head] = key_mod[:, span]
        vectors[4, head] = recept[:, span]

    lanes = lax.broadcasted_iota(jnp.int32, (head_size, seq_count), 1)

    def update(seq, carry):
        here = lanes == seq
        for head in range(heads):
            span = slice(head * head_size, (head + 1) * head_size)
            row = pl.ds(seq, 1)
            state = state_buf[seq, head]
            removed = jnp.sum(state * vectors[1, head, row, :], axis=1, keepdims=True)
            column = jnp.sum(jnp.where(here, value_t[span, :], 0.0), axis=1, keepdims=True)
            state = (
                state * vectors[0, head, row, :]
                - removed * vectors[2, head, row, :]
                + column * vectors[3, head, row, :]
            )
            out_buf[seq, head] = state
            mixed = jnp.sum(state * vectors[4, head, row, :], axis=1, keepdims=True)
            mixed_t[span, :] = jnp.where(here, mixed, mixed_t[span, :])
        return carry

    mixed_t[...] = jnp.zeros_like(mixed_t)
    for index in range(n_chunks):
        state_loads[index].wait()
        lax.fori_loop(index * per_chunk, (index + 1) * per_chunk, update, 0, unroll=2)
        state_stores[index].start()
    mixed_ref[...] = mixed_t[...].T.astype(bf16)
    for store in state_stores:
        store.wait()


def moe_kernel(
    ep_count,
    block_rows,
    mixed_ref,
    w_out_hbm,
    tokens_ref,
    norm_ref,
    router_group_ref,
    router_expert_ref,
    routes_ref,
    gate_hbm,
    up_hbm,
    down_hbm,
    moe_ref,
    mid_ref,
    gate_ref,
    up_ref,
    down_ref,
    w_out_ref,
    part_buf,
    part_recv,
    mid_buf,
    norm_buf,
    send_buf,
    rows_buf,
    hidden_buf,
    term_send,
    term_own,
    term_recv,
    result_buf,
    back_buf,
    part_sems,
    out_send_sems,
    out_recv_sems,
    pair_send_sems,
    pair_recv_sems,
    term_send_sems,
    term_recv_sems,
    back_send_sems,
    back_recv_sems,
    load_sems,
):
    f32 = jnp.float32
    bf16 = jnp.bfloat16
    me = lax.axis_index("ep")
    core = lax.axis_index("tp")
    other = 1 - core
    seq_count, width = tokens_ref.shape
    half = width // 2
    cap = send_buf.shape[1]
    total_rows = ep_count * cap
    per_block = block_rows // cap
    n_blocks = total_rows // block_rows
    mesh_ids = pl.DeviceIdType.MESH

    def peer_at(step):
        return lax.rem(me + step, ep_count)

    def step_at(index):
        return 1 + lax.rem(index + ep_count // 2 - 1, ep_count - 1)

    barrier = pltpu.get_barrier_semaphore()
    pl.semaphore_signal(barrier, inc=1, device_id=(me, other), device_id_type=mesh_ids)

    def greet(step, carry):
        pl.semaphore_signal(
            barrier, inc=1, device_id=(peer_at(step), core), device_id_type=mesh_ids
        )
        return carry

    lax.fori_loop(1, ep_count, greet, 0)

    loads = [
        pltpu.make_async_copy(w_out_hbm, w_out_ref, load_sems.at[0]),
        pltpu.make_async_copy(gate_hbm.at[0], gate_ref, load_sems.at[1]),
        pltpu.make_async_copy(up_hbm.at[0], up_ref, load_sems.at[2]),
        pltpu.make_async_copy(down_hbm.at[0, :, pl.ds(0, half)], down_ref.at[0], load_sems.at[3]),
        pltpu.make_async_copy(down_hbm.at[0, :, pl.ds(half, half)], down_ref.at[1], load_sems.at[4]),
    ]
    for load in loads:
        load.start()

    n_groups = router_group_ref.shape[0]
    expert_ids = lax.broadcasted_iota(jnp.int32, (ep_count, seq_count), 0)
    uses = jnp.zeros((ep_count, seq_count), f32)
    for index in range(routes_ref.shape[0]):
        uses += jnp.where(routes_ref[index : index + 1, :] == expert_ids, 1.0, 0.0)
    group_ids = lax.broadcasted_iota(jnp.int32, (n_groups, seq_count), 0)
    group_hit = jnp.where(
        routes_ref[0:1, :] // (ep_count // n_groups) == group_ids, 1.0, 0.0
    )
    row_ids = lax.broadcasted_iota(jnp.int32, (seq_count, seq_count), 0)
    column_ids = lax.broadcasted_iota(jnp.int32, (seq_count, seq_count), 1)
    earlier = jnp.where(row_ids < column_ids, 1.0, 0.0).astype(bf16)
    position = jnp.dot(uses.astype(bf16), earlier, preferred_element_type=f32)
    slots = jnp.where(uses > 0.5, position, -1.0).astype(bf16)
    slot_rows = lax.broadcasted_iota(jnp.int32, (total_rows, ep_count), 0)
    slot_experts = lax.broadcasted_iota(jnp.int32, (total_rows, ep_count), 1)
    spread = jnp.where(slot_rows // cap == slot_experts, 1.0, 0.0).astype(bf16)
    slot_of_row = lax.broadcasted_iota(jnp.int32, (total_rows, seq_count), 0) % cap
    hits = jnp.dot(spread, slots, preferred_element_type=f32) == slot_of_row.astype(f32)
    chooser = jnp.where(hits, 1.0, 0.0)
    placement = chooser.astype(bf16)

    loads[0].wait()
    for index in range(2):
        columns = slice(index * half, (index + 1) * half)
        part_buf[index] = jnp.dot(
            mixed_ref[...], w_out_ref[:, columns], preferred_element_type=f32
        )
    pl.semaphore_wait(barrier, ep_count)

    def pair_copy(source, target, send_sem, recv_sem):
        return pltpu.make_async_remote_copy(
            src_ref=source,
            dst_ref=target,
            send_sem=send_sem,
            recv_sem=recv_sem,
            device_id=(me, other),
            device_id_type=mesh_ids,
        )

    part_copy = pair_copy(part_buf, part_recv, part_sems.at[0], part_sems.at[1])
    part_copy.start()
    part_copy.wait()

    squares = jnp.zeros((seq_count, 1), f32)
    for index in range(2):
        columns = slice(index * half, (index + 1) * half)
        mixer_out = (part_buf[index] + part_recv[index]).astype(bf16)
        mid = (tokens_ref[:, columns].astype(f32) + mixer_out.astype(f32)).astype(bf16)
        mid_buf[index] = mid
        mid32 = mid.astype(f32)
        squares = squares + jnp.sum(mid32 * mid32, axis=1, keepdims=True)
    factor = lax.rsqrt(squares / width + 1e-06)
    for index in range(2):
        columns = slice(index * half, (index + 1) * half)
        norm_buf[index] = (
            mid_buf[index].astype(f32) * factor * norm_ref[columns].reshape(1, half).astype(f32)
        ).astype(bf16)

    own_norm = norm_buf[core]
    for index in range(n_blocks):
        rows = jnp.dot(
            placement[index * block_rows : (index + 1) * block_rows, :],
            own_norm,
            preferred_element_type=f32,
        ).astype(bf16)
        send_buf[index * per_block : (index + 1) * per_block] = rows.reshape(per_block, cap, half)

    def out_copy(step):
        peer = peer_at(step)
        return pltpu.make_async_remote_copy(
            src_ref=send_buf.at[peer],
            dst_ref=rows_buf.at[core, me],
            send_sem=out_send_sems.at[step],
            recv_sem=out_recv_sems.at[step],
            device_id=(peer, core),
            device_id_type=mesh_ids,
        )

    def rows_copy(step):
        source = lax.rem(me + ep_count - step, ep_count)
        return pair_copy(
            rows_buf.at[core, source],
            rows_buf.at[core, source],
            pair_send_sems.at[step],
            pair_recv_sems.at[step],
        )

    def rows_arrival(step):
        source = lax.rem(me + ep_count - step, ep_count)
        return pair_copy(
            rows_buf.at[other, source],
            rows_buf.at[other, source],
            pair_send_sems.at[step],
            pair_recv_sems.at[step],
        )

    def start_out(index, carry):
        out_copy(step_at(index)).start()
        return carry

    lax.fori_loop(0, ep_count - 1, start_out, 0)
    rows_buf[core, me] = send_buf[me]
    rows_copy(0).start()

    rows_dims = (((1,), (1,)), ((), ()))
    group_logit = jnp.zeros(group_hit.shape, f32)
    expert_logit = jnp.zeros(uses.shape, f32)
    for index in range(2):
        columns = slice(index * half, (index + 1) * half)
        group_logit += lax.dot_general(
            router_group_ref[:, columns], norm_buf[index], rows_dims, preferred_element_type=f32
        )
        expert_logit += lax.dot_general(
            router_expert_ref[:, columns], norm_buf[index], rows_dims, preferred_element_type=f32
        )
    group_prob = jax.nn.sigmoid(jnp.sum(group_logit * group_hit, axis=0, keepdims=True))
    scores = jax.nn.sigmoid(expert_logit) * uses
    weights = group_prob * scores / jnp.sum(scores, axis=0, keepdims=True)
    weights_high = weights.astype(bf16)
    weights_low = (weights - weights_high.astype(f32)).astype(bf16)
    combine_high = (jnp.dot(spread, weights_high, preferred_element_type=f32) * chooser).T
    combine_low = (jnp.dot(spread, weights_low, preferred_element_type=f32) * chooser).T
    combine_high = combine_high.astype(bf16)
    combine_low = combine_low.astype(bf16)
    mid_ref[...] = mid_buf[core]

    def relay(index, carry):
        step = step_at(ep_count - 2 - index)
        out_copy(step).wait_recv()
        rows_copy(step).start()
        return carry

    lax.fori_loop(0, ep_count - 1, relay, 0)

    def arrive(step, carry):
        rows_arrival(step).wait_recv()
        return carry

    lax.fori_loop(0, ep_count, arrive, 0)

    for load in loads[1:]:
        load.wait()
    for index in range(n_blocks):
        experts = slice(index * per_block, (index + 1) * per_block)
        gate_part = jnp.zeros((block_rows, gate_ref.shape[1]), f32)
        up_part = jnp.zeros((block_rows, gate_ref.shape[1]), f32)
        for piece in range(2):
            columns = slice(piece * half, (piece + 1) * half)
            rows = rows_buf[piece, experts].reshape(block_rows, half)
            gate_part += jnp.dot(rows, gate_ref[columns, :], preferred_element_type=f32)
            up_part += jnp.dot(rows, up_ref[columns, :], preferred_element_type=f32)
        hidden = (gate_part / (1.0 + jnp.exp(-gate_part)) * up_part).astype(bf16)
        hidden_buf[experts] = hidden.reshape(per_block, cap, gate_ref.shape[1])

    n_parts = term_send.shape[0]
    per_part = ep_count // n_parts
    first_part = me // per_part

    def part_at(index):
        return lax.rem(first_part + index + n_parts // 2, n_parts)

    def term_copy(part):
        return pair_copy(
            term_send.at[part],
            term_recv.at[part],
            term_send_sems.at[part],
            term_recv_sems.at[part],
        )

    def part_term(part, which):
        hidden = hidden_buf[pl.ds(part * per_part, per_part)]
        hidden = hidden.reshape(per_part * cap, gate_ref.shape[1])
        term = jnp.dot(hidden, down_ref[which], preferred_element_type=f32)
        return term.astype(bf16).reshape(per_part, cap, half)

    def back_copy(peer):
        return pltpu.make_async_remote_copy(
            src_ref=result_buf.at[peer],
            dst_ref=back_buf.at[me],
            send_sem=back_send_sems.at[peer],
            recv_sem=back_recv_sems.at[me],
            device_id=(peer, core),
            device_id_type=mesh_ids,
        )

    def back_arrival(peer):
        return pltpu.make_async_remote_copy(
            src_ref=result_buf.at[peer],
            dst_ref=back_buf.at[peer],
            send_sem=back_send_sems.at[peer],
            recv_sem=back_recv_sems.at[peer],
            device_id=(peer, core),
            device_id_type=mesh_ids,
        )

    def send_terms(index, carry):
        part = part_at(index)
        term_send[part] = part_term(part, other)
        term_copy(part).start()
        return carry

    lax.fori_loop(0, n_parts, send_terms, 0)

    def own_terms(index, carry):
        part = part_at(index)
        term_own[part] = part_term(part, core)
        return carry

    lax.fori_loop(0, n_parts, own_terms, 0)

    def finish_part(index, carry):
        part = part_at(index)
        term_copy(part).wait_recv()
        total = term_own[part].astype(f32) + term_recv[part].astype(f32)
        result_buf[pl.ds(part * per_part, per_part)] = total.astype(bf16)

        def start_back(inner, carry_inner):
            peer = part * per_part + inner

            @pl.when(peer != me)
            def _():
                back_copy(peer).start()

            return carry_inner

        lax.fori_loop(0, per_part, start_back, 0)
        return carry

    lax.fori_loop(0, n_parts, finish_part, 0)
    back_buf[me] = result_buf[me]

    def finish_sends(step, carry):
        out_copy(step).wait_send()
        back_arrival(peer_at(step)).wait_recv()
        back_copy(peer_at(step)).wait_send()
        return carry

    lax.fori_loop(1, ep_count, finish_sends, 0)

    def finish_pair(step, carry):
        rows_copy(step).wait_send()
        return carry

    lax.fori_loop(0, ep_count, finish_pair, 0)

    def finish_terms(part, carry):
        term_copy(part).wait_send()
        return carry

    lax.fori_loop(0, n_parts, finish_terms, 0)

    back = back_buf[...].reshape(total_rows, half)
    moe_out = jnp.dot(combine_high, back, preferred_element_type=f32)
    moe_out += jnp.dot(combine_low, back, preferred_element_type=f32)
    moe_ref[...] = moe_out


def shards(
    tokens_in,
    state_in,
    norm_mix,
    w_recept,
    w_key,
    w_value,
    decay_down,
    decay_up,
    decay_base,
    iclr_down,
    iclr_up,
    iclr_base,
    key_scale,
    key_mix,
    w_out,
    norm_moe,
    router_group,
    router_expert,
    routes,
    expert_gate,
    expert_up,
    expert_down,
):
    f32 = jnp.float32
    bf16 = jnp.bfloat16
    seq_count, width_model = tokens_in.shape
    heads_here, head_size = state_in.shape[1], state_in.shape[3]
    channels = heads_here * head_size
    tp_count = lax.axis_size("tp")
    ep_count = lax.axis_size("ep")
    dma = pltpu.SemaphoreType.DMA
    vmem = pl.BlockSpec(memory_space=pltpu.VMEM)
    anywhere = pl.BlockSpec(memory_space=pl.ANY)
    n_chunks = 4 if seq_count % 4 == 0 else 1
    mixed, state_out = pl.pallas_call(
        mixer_kernel,
        out_shape=(
            jax.ShapeDtypeStruct((seq_count, channels), bf16),
            jax.ShapeDtypeStruct(state_in.shape, f32),
        ),
        in_specs=[vmem] * 2 + [anywhere] * 3 + [vmem] * 8 + [anywhere],
        out_specs=(vmem, anywhere),
        scratch_shapes=[
            pltpu.VMEM((3, width_model, channels), bf16),
            pltpu.VMEM(state_in.shape, f32),
            pltpu.VMEM(state_in.shape, f32),
            pltpu.VMEM((5, heads_here, seq_count, head_size), f32),
            pltpu.VMEM((channels, seq_count), f32),
            pltpu.VMEM((channels, seq_count), f32),
            dma((3,)),
            dma((n_chunks,)),
            dma((n_chunks,)),
        ],
        compiler_params=pltpu.CompilerParams(vmem_limit_bytes=60 * 1024 * 1024),
    )(
        tokens_in,
        norm_mix,
        w_recept,
        w_key,
        w_value,
        decay_down.T,
        decay_up,
        decay_base,
        iclr_down.T,
        iclr_up,
        iclr_base,
        key_scale,
        key_mix,
        state_in,
    )
    top_count = routes.shape[1]
    half_width = width_model // tp_count
    limit = max(2, 2 * seq_count * top_count // ep_count)
    cap = -(-limit // 16) * 16
    block_rows = min(ep_count * cap, 256)
    n_parts = min(4, ep_count)
    per_part = ep_count // n_parts
    hidden_width = expert_gate.shape[2]
    moe_out, mid_half = pl.pallas_call(
        functools.partial(moe_kernel, ep_count, block_rows),
        out_shape=(
            jax.ShapeDtypeStruct((seq_count, half_width), f32),
            jax.ShapeDtypeStruct((seq_count, half_width), bf16),
        ),
        in_specs=[vmem, anywhere] + [vmem] * 5 + [anywhere] * 3,
        out_specs=(vmem, vmem),
        scratch_shapes=[
            pltpu.VMEM((width_model, hidden_width), bf16),
            pltpu.VMEM((width_model, hidden_width), bf16),
            pltpu.VMEM((tp_count, hidden_width, half_width), bf16),
            pltpu.VMEM(w_out.shape, bf16),
            pltpu.VMEM((tp_count, seq_count, half_width), f32),
            pltpu.VMEM((tp_count, seq_count, half_width), f32),
            pltpu.VMEM((tp_count, seq_count, half_width), bf16),
            pltpu.VMEM((tp_count, seq_count, half_width), bf16),
            pltpu.VMEM((ep_count, cap, half_width), bf16),
            pltpu.VMEM((tp_count, ep_count, cap, half_width), bf16),
            pltpu.VMEM((ep_count, cap, hidden_width), bf16),
            pltpu.VMEM((n_parts, per_part, cap, half_width), bf16),
            pltpu.VMEM((n_parts, per_part, cap, half_width), bf16),
            pltpu.VMEM((n_parts, per_part, cap, half_width), bf16),
            pltpu.VMEM((ep_count, cap, half_width), bf16),
            pltpu.VMEM((ep_count, cap, half_width), bf16),
            dma((2,)),
            dma((ep_count,)),
            dma((ep_count,)),
            dma((ep_count,)),
            dma((ep_count,)),
            dma((n_parts,)),
            dma((n_parts,)),
            dma((ep_count,)),
            dma((ep_count,)),
            dma((5,)),
        ],
        compiler_params=pltpu.CompilerParams(
            collective_id=0, has_side_effects=True, vmem_limit_bytes=60 * 1024 * 1024
        ),
    )(
        mixed,
        w_out,
        tokens_in,
        norm_moe,
        router_group.T,
        router_expert.T,
        routes.T,
        expert_gate,
        expert_up,
        expert_down,
    )
    layer_out = (mid_half.astype(f32) + moe_out).astype(bf16)
    return (layer_out, state_out)


def solution(mesh):
    in_specs = (
        P("ep", None),
        P("ep", "tp", None, None),
        P(),
        P(None, "tp"),
        P(None, "tp"),
        P(None, "tp"),
        P(),
        P(None, "tp"),
        P("tp"),
        P(),
        P(None, "tp"),
        P("tp"),
        P("tp"),
        P("tp"),
        P("tp", None),
        P(),
        P(),
        P(),
        P("ep", None),
        P("ep", None, "tp"),
        P("ep", None, "tp"),
        P("ep", "tp", None),
    )
    out_specs = (P("ep", "tp"), P("ep", "tp", None, None))
    return jax.shard_map(shards, mesh=mesh, in_specs=in_specs, out_specs=out_specs, check_vma=False)
```

```python
import functools

import jax
import jax.numpy as jnp
from jax import lax
from jax.experimental import pallas as pl
from jax.experimental.pallas import tpu as pltpu
from jax.sharding import PartitionSpec as P


def mixer_kernel(
    tokens_ref,
    norm_ref,
    w_recept_hbm,
    w_key_hbm,
    w_value_hbm,
    decay_down_ref,
    decay_up_ref,
    decay_base_ref,
    iclr_down_ref,
    iclr_up_ref,
    iclr_base_ref,
    key_scale_ref,
    key_mix_ref,
    state_hbm,
    mixed_ref,
    state_out_hbm,
    weights,
    state_buf,
    out_buf,
    vectors,
    value_t,
    mixed_t,
    weight_sems,
    in_sems,
    out_sems,
):
    f32 = jnp.float32
    bf16 = jnp.bfloat16
    seq_count, width = tokens_ref.shape
    heads, head_size = state_hbm.shape[1], state_hbm.shape[3]
    channels = heads * head_size
    n_chunks = in_sems.shape[0]
    per_chunk = seq_count // n_chunks
    rows_dims = (((1,), (1,)), ((), ()))
    weight_loads = [
        pltpu.make_async_copy(source, weights.at[index], weight_sems.at[index])
        for index, source in enumerate((w_key_hbm, w_value_hbm, w_recept_hbm))
    ]
    for load in weight_loads:
        load.start()
    state_loads = []
    state_stores = []
    for index in range(n_chunks):
        span = pl.ds(index * per_chunk, per_chunk)
        state_loads.append(
            pltpu.make_async_copy(state_hbm.at[span], state_buf.at[span], in_sems.at[index])
        )
        state_stores.append(
            pltpu.make_async_copy(out_buf.at[span], state_out_hbm.at[span], out_sems.at[index])
        )
        state_loads[index].start()

    tokens = tokens_ref[...].astype(f32)
    factor = lax.rsqrt(jnp.mean(tokens * tokens, axis=1, keepdims=True) + 1e-06)
    normed = (tokens * factor * norm_ref[...].reshape(1, width).astype(f32)).astype(bf16)
    decay_low = jnp.tanh(
        lax.dot_general(normed, decay_down_ref[...], rows_dims, preferred_element_type=f32)
    ).astype(bf16)
    iclr_low = lax.dot_general(
        normed, iclr_down_ref[...], rows_dims, preferred_element_type=f32
    ).astype(bf16)
    decay_in = decay_base_ref[...].reshape(1, channels) + jnp.dot(
        decay_low, decay_up_ref[...], preferred_element_type=f32
    )
    decays = jnp.exp(-jnp.exp(jnp.float32(-0.5)) * jax.nn.sigmoid(decay_in))
    rate = jax.nn.sigmoid(
        iclr_base_ref[...].reshape(1, channels)
        + jnp.dot(iclr_low, iclr_up_ref[...], preferred_element_type=f32)
    )
    projected = []
    for index in range(3):
        weight_loads[index].wait()
        rows = jnp.dot(normed, weights[index], preferred_element_type=f32)
        projected.append(rows.astype(bf16).astype(f32))
    key, value, recept = projected
    value_t[...] = value.T
    scaled = key * key_scale_ref[...].reshape(1, channels).astype(f32)
    key_mod = key * (1.0 + (rate - 1.0) * key_mix_ref[...].reshape(1, channels).astype(f32))
    for head in range(heads):
        span = slice(head * head_size, (head + 1) * head_size)
        part = scaled[:, span]
        unit = part * lax.rsqrt(jnp.sum(part * part, axis=1, keepdims=True) + 1e-06)
        vectors[0, head] = decays[:, span]
        vectors[1, head] = unit
        vectors[2, head] = unit * rate[:, span]
        vectors[3, head] = key_mod[:, span]
        vectors[4, head] = recept[:, span]

    lanes = lax.broadcasted_iota(jnp.int32, (head_size, seq_count), 1)

    def update(seq, carry):
        here = lanes == seq
        for head in range(heads):
            span = slice(head * head_size, (head + 1) * head_size)
            row = pl.ds(seq, 1)
            state = state_buf[seq, head]
            removed = jnp.sum(state * vectors[1, head, row, :], axis=1, keepdims=True)
            column = jnp.sum(jnp.where(here, value_t[span, :], 0.0), axis=1, keepdims=True)
            state = (
                state * vectors[0, head, row, :]
                - removed * vectors[2, head, row, :]
                + column * vectors[3, head, row, :]
            )
            out_buf[seq, head] = state
            mixed = jnp.sum(state * vectors[4, head, row, :], axis=1, keepdims=True)
            mixed_t[span, :] = jnp.where(here, mixed, mixed_t[span, :])
        return carry

    mixed_t[...] = jnp.zeros_like(mixed_t)
    for index in range(n_chunks):
        state_loads[index].wait()
        lax.fori_loop(index * per_chunk, (index + 1) * per_chunk, update, 0, unroll=4)
        state_stores[index].start()
    mixed_ref[...] = mixed_t[...].T.astype(bf16)
    for store in state_stores:
        store.wait()


def moe_kernel(
    ep_count,
    block_rows,
    mixed_ref,
    w_out_hbm,
    tokens_ref,
    norm_ref,
    router_group_ref,
    router_expert_ref,
    routes_ref,
    gate_hbm,
    up_hbm,
    down_hbm,
    moe_ref,
    mid_ref,
    gate_ref,
    up_ref,
    down_ref,
    w_out_ref,
    part_buf,
    part_recv,
    mid_buf,
    norm_buf,
    send_buf,
    rows_buf,
    hidden_buf,
    term_send,
    term_own,
    term_recv,
    result_buf,
    back_buf,
    part_sems,
    out_send_sems,
    out_recv_sems,
    pair_send_sems,
    pair_recv_sems,
    term_send_sems,
    term_recv_sems,
    back_send_sems,
    back_recv_sems,
    load_sems,
):
    f32 = jnp.float32
    bf16 = jnp.bfloat16
    me = lax.axis_index("ep")
    core = lax.axis_index("tp")
    other = 1 - core
    seq_count, width = tokens_ref.shape
    half = width // 2
    cap = send_buf.shape[1]
    total_rows = ep_count * cap
    per_block = block_rows // cap
    n_blocks = total_rows // block_rows
    mesh_ids = pl.DeviceIdType.MESH

    def peer_at(step):
        return lax.rem(me + step, ep_count)

    def step_at(index):
        return 1 + lax.rem(index + ep_count // 2 - 1, ep_count - 1)

    barrier = pltpu.get_barrier_semaphore()
    pl.semaphore_signal(barrier, inc=1, device_id=(me, other), device_id_type=mesh_ids)

    def greet(step, carry):
        pl.semaphore_signal(
            barrier, inc=1, device_id=(peer_at(step), core), device_id_type=mesh_ids
        )
        return carry

    lax.fori_loop(1, ep_count, greet, 0)

    loads = [
        pltpu.make_async_copy(w_out_hbm, w_out_ref, load_sems.at[0]),
        pltpu.make_async_copy(gate_hbm.at[0], gate_ref, load_sems.at[1]),
        pltpu.make_async_copy(up_hbm.at[0], up_ref, load_sems.at[2]),
        pltpu.make_async_copy(down_hbm.at[0, :, pl.ds(0, half)], down_ref.at[0], load_sems.at[3]),
        pltpu.make_async_copy(down_hbm.at[0, :, pl.ds(half, half)], down_ref.at[1], load_sems.at[4]),
    ]
    for load in loads:
        load.start()

    n_groups = router_group_ref.shape[0]
    expert_ids = lax.broadcasted_iota(jnp.int32, (ep_count, seq_count), 0)
    uses = jnp.zeros((ep_count, seq_count), f32)
    for index in range(routes_ref.shape[0]):
        uses += jnp.where(routes_ref[index : index + 1, :] == expert_ids, 1.0, 0.0)
    group_ids = lax.broadcasted_iota(jnp.int32, (n_groups, seq_count), 0)
    group_hit = jnp.where(
        routes_ref[0:1, :] // (ep_count // n_groups) == group_ids, 1.0, 0.0
    )
    row_ids = lax.broadcasted_iota(jnp.int32, (seq_count, seq_count), 0)
    column_ids = lax.broadcasted_iota(jnp.int32, (seq_count, seq_count), 1)
    earlier = jnp.where(row_ids < column_ids, 1.0, 0.0).astype(bf16)
    position = jnp.dot(uses.astype(bf16), earlier, preferred_element_type=f32)
    slots = jnp.where(uses > 0.5, position, -1.0).astype(bf16)
    slot_rows = lax.broadcasted_iota(jnp.int32, (total_rows, ep_count), 0)
    slot_experts = lax.broadcasted_iota(jnp.int32, (total_rows, ep_count), 1)
    spread = jnp.where(slot_rows // cap == slot_experts, 1.0, 0.0).astype(bf16)
    slot_of_row = lax.broadcasted_iota(jnp.int32, (total_rows, seq_count), 0) % cap
    hits = jnp.dot(spread, slots, preferred_element_type=f32) == slot_of_row.astype(f32)
    chooser = jnp.where(hits, 1.0, 0.0)
    placement = chooser.astype(bf16)

    loads[0].wait()
    for index in range(2):
        columns = slice(index * half, (index + 1) * half)
        part_buf[index] = jnp.dot(
            mixed_ref[...], w_out_ref[:, columns], preferred_element_type=f32
        )
    pl.semaphore_wait(barrier, ep_count)

    def pair_copy(source, target, send_sem, recv_sem):
        return pltpu.make_async_remote_copy(
            src_ref=source,
            dst_ref=target,
            send_sem=send_sem,
            recv_sem=recv_sem,
            device_id=(me, other),
            device_id_type=mesh_ids,
        )

    part_copy = pair_copy(part_buf, part_recv, part_sems.at[0], part_sems.at[1])
    part_copy.start()
    part_copy.wait()

    squares = jnp.zeros((seq_count, 1), f32)
    for index in range(2):
        columns = slice(index * half, (index + 1) * half)
        mixer_out = (part_buf[index] + part_recv[index]).astype(bf16)
        mid = (tokens_ref[:, columns].astype(f32) + mixer_out.astype(f32)).astype(bf16)
        mid_buf[index] = mid
        mid32 = mid.astype(f32)
        squares = squares + jnp.sum(mid32 * mid32, axis=1, keepdims=True)
    factor = lax.rsqrt(squares / width + 1e-06)
    for index in range(2):
        columns = slice(index * half, (index + 1) * half)
        norm_buf[index] = (
            mid_buf[index].astype(f32) * factor * norm_ref[columns].reshape(1, half).astype(f32)
        ).astype(bf16)

    own_norm = norm_buf[core]
    for index in range(n_blocks):
        rows = jnp.dot(
            placement[index * block_rows : (index + 1) * block_rows, :],
            own_norm,
            preferred_element_type=f32,
        ).astype(bf16)
        send_buf[index * per_block : (index + 1) * per_block] = rows.reshape(per_block, cap, half)

    def out_copy(step):
        peer = peer_at(step)
        return pltpu.make_async_remote_copy(
            src_ref=send_buf.at[peer],
            dst_ref=rows_buf.at[core, me],
            send_sem=out_send_sems.at[step],
            recv_sem=out_recv_sems.at[step],
            device_id=(peer, core),
            device_id_type=mesh_ids,
        )

    def rows_copy(step):
        source = lax.rem(me + ep_count - step, ep_count)
        return pair_copy(
            rows_buf.at[core, source],
            rows_buf.at[core, source],
            pair_send_sems.at[step],
            pair_recv_sems.at[step],
        )

    def rows_arrival(step):
        source = lax.rem(me + ep_count - step, ep_count)
        return pair_copy(
            rows_buf.at[other, source],
            rows_buf.at[other, source],
            pair_send_sems.at[step],
            pair_recv_sems.at[step],
        )

    def start_out(index, carry):
        out_copy(step_at(index)).start()
        return carry

    lax.fori_loop(0, ep_count - 1, start_out, 0)
    rows_buf[core, me] = send_buf[me]
    rows_copy(0).start()

    rows_dims = (((1,), (1,)), ((), ()))
    group_logit = jnp.zeros(group_hit.shape, f32)
    expert_logit = jnp.zeros(uses.shape, f32)
    for index in range(2):
        columns = slice(index * half, (index + 1) * half)
        group_logit += lax.dot_general(
            router_group_ref[:, columns], norm_buf[index], rows_dims, preferred_element_type=f32
        )
        expert_logit += lax.dot_general(
            router_expert_ref[:, columns], norm_buf[index], rows_dims, preferred_element_type=f32
        )
    group_prob = jax.nn.sigmoid(jnp.sum(group_logit * group_hit, axis=0, keepdims=True))
    scores = jax.nn.sigmoid(expert_logit) * uses
    weights = group_prob * scores / jnp.sum(scores, axis=0, keepdims=True)
    weights_high = weights.astype(bf16)
    weights_low = (weights - weights_high.astype(f32)).astype(bf16)
    combine_high = (jnp.dot(spread, weights_high, preferred_element_type=f32) * chooser).T
    combine_low = (jnp.dot(spread, weights_low, preferred_element_type=f32) * chooser).T
    combine_high = combine_high.astype(bf16)
    combine_low = combine_low.astype(bf16)
    mid_ref[...] = mid_buf[core]

    def relay(index, carry):
        step = step_at(index)
        out_copy(step).wait_recv()
        rows_copy(step).start()
        return carry

    lax.fori_loop(0, ep_count - 1, relay, 0)

    def arrive(step, carry):
        rows_arrival(step).wait_recv()
        return carry

    lax.fori_loop(0, ep_count, arrive, 0)

    for load in loads[1:]:
        load.wait()
    for index in range(n_blocks):
        experts = slice(index * per_block, (index + 1) * per_block)
        gate_part = jnp.zeros((block_rows, gate_ref.shape[1]), f32)
        up_part = jnp.zeros((block_rows, gate_ref.shape[1]), f32)
        for piece in range(2):
            columns = slice(piece * half, (piece + 1) * half)
            rows = rows_buf[piece, experts].reshape(block_rows, half)
            gate_part += jnp.dot(rows, gate_ref[columns, :], preferred_element_type=f32)
            up_part += jnp.dot(rows, up_ref[columns, :], preferred_element_type=f32)
        hidden = (gate_part / (1.0 + jnp.exp(-gate_part)) * up_part).astype(bf16)
        hidden_buf[experts] = hidden.reshape(per_block, cap, gate_ref.shape[1])

    n_parts = term_send.shape[0]
    per_part = ep_count // n_parts
    first_part = me // per_part

    def part_at(index):
        return lax.rem(first_part + index + n_parts // 2, n_parts)

    def term_copy(part):
        return pair_copy(
            term_send.at[part],
            term_recv.at[part],
            term_send_sems.at[part],
            term_recv_sems.at[part],
        )

    def part_term(part, which):
        hidden = hidden_buf[pl.ds(part * per_part, per_part)]
        hidden = hidden.reshape(per_part * cap, gate_ref.shape[1])
        term = jnp.dot(hidden, down_ref[which], preferred_element_type=f32)
        return term.astype(bf16).reshape(per_part, cap, half)

    def back_copy(peer):
        return pltpu.make_async_remote_copy(
            src_ref=result_buf.at[peer],
            dst_ref=back_buf.at[me],
            send_sem=back_send_sems.at[peer],
            recv_sem=back_recv_sems.at[me],
            device_id=(peer, core),
            device_id_type=mesh_ids,
        )

    def back_arrival(peer):
        return pltpu.make_async_remote_copy(
            src_ref=result_buf.at[peer],
            dst_ref=back_buf.at[peer],
            send_sem=back_send_sems.at[peer],
            recv_sem=back_recv_sems.at[peer],
            device_id=(peer, core),
            device_id_type=mesh_ids,
        )

    def send_terms(index, carry):
        part = part_at(index)
        term_send[part] = part_term(part, other)
        term_copy(part).start()
        return carry

    lax.fori_loop(0, n_parts, send_terms, 0)

    def own_terms(index, carry):
        part = part_at(index)
        term_own[part] = part_term(part, core)
        return carry

    lax.fori_loop(0, n_parts, own_terms, 0)

    def finish_part(index, carry):
        part = part_at(index)
        term_copy(part).wait_recv()
        total = term_own[part].astype(f32) + term_recv[part].astype(f32)
        result_buf[pl.ds(part * per_part, per_part)] = total.astype(bf16)

        def start_back(inner, carry_inner):
            peer = part * per_part + inner

            @pl.when(peer != me)
            def _():
                back_copy(peer).start()

            return carry_inner

        lax.fori_loop(0, per_part, start_back, 0)
        return carry

    lax.fori_loop(0, n_parts, finish_part, 0)
    back_buf[me] = result_buf[me]

    def finish_sends(step, carry):
        out_copy(step).wait_send()
        back_arrival(peer_at(step)).wait_recv()
        back_copy(peer_at(step)).wait_send()
        return carry

    lax.fori_loop(1, ep_count, finish_sends, 0)

    def finish_pair(step, carry):
        rows_copy(step).wait_send()
        return carry

    lax.fori_loop(0, ep_count, finish_pair, 0)

    def finish_terms(part, carry):
        term_copy(part).wait_send()
        return carry

    lax.fori_loop(0, n_parts, finish_terms, 0)

    back = back_buf[...].reshape(total_rows, half)
    moe_out = jnp.dot(combine_high, back, preferred_element_type=f32)
    moe_out += jnp.dot(combine_low, back, preferred_element_type=f32)
    moe_ref[...] = moe_out


def shards(
    tokens_in,
    state_in,
    norm_mix,
    w_recept,
    w_key,
    w_value,
    decay_down,
    decay_up,
    decay_base,
    iclr_down,
    iclr_up,
    iclr_base,
    key_scale,
    key_mix,
    w_out,
    norm_moe,
    router_group,
    router_expert,
    routes,
    expert_gate,
    expert_up,
    expert_down,
):
    f32 = jnp.float32
    bf16 = jnp.bfloat16
    seq_count, width_model = tokens_in.shape
    heads_here, head_size = state_in.shape[1], state_in.shape[3]
    channels = heads_here * head_size
    tp_count = lax.axis_size("tp")
    ep_count = lax.axis_size("ep")
    dma = pltpu.SemaphoreType.DMA
    vmem = pl.BlockSpec(memory_space=pltpu.VMEM)
    anywhere = pl.BlockSpec(memory_space=pl.ANY)
    n_chunks = 4 if seq_count % 4 == 0 else 1
    mixed, state_out = pl.pallas_call(
        mixer_kernel,
        out_shape=(
            jax.ShapeDtypeStruct((seq_count, channels), bf16),
            jax.ShapeDtypeStruct(state_in.shape, f32),
        ),
        in_specs=[vmem] * 2 + [anywhere] * 3 + [vmem] * 8 + [anywhere],
        out_specs=(vmem, anywhere),
        scratch_shapes=[
            pltpu.VMEM((3, width_model, channels), bf16),
            pltpu.VMEM(state_in.shape, f32),
            pltpu.VMEM(state_in.shape, f32),
            pltpu.VMEM((5, heads_here, seq_count, head_size), f32),
            pltpu.VMEM((channels, seq_count), f32),
            pltpu.VMEM((channels, seq_count), f32),
            dma((3,)),
            dma((n_chunks,)),
            dma((n_chunks,)),
        ],
        compiler_params=pltpu.CompilerParams(vmem_limit_bytes=60 * 1024 * 1024),
    )(
        tokens_in,
        norm_mix,
        w_recept,
        w_key,
        w_value,
        decay_down.T,
        decay_up,
        decay_base,
        iclr_down.T,
        iclr_up,
        iclr_base,
        key_scale,
        key_mix,
        state_in,
    )
    top_count = routes.shape[1]
    half_width = width_model // tp_count
    limit = max(2, 2 * seq_count * top_count // ep_count)
    cap = -(-limit // 16) * 16
    block_rows = min(ep_count * cap, 256)
    n_parts = min(4, ep_count)
    per_part = ep_count // n_parts
    hidden_width = expert_gate.shape[2]
    moe_out, mid_half = pl.pallas_call(
        functools.partial(moe_kernel, ep_count, block_rows),
        out_shape=(
            jax.ShapeDtypeStruct((seq_count, half_width), f32),
            jax.ShapeDtypeStruct((seq_count, half_width), bf16),
        ),
        in_specs=[vmem, anywhere] + [vmem] * 5 + [anywhere] * 3,
        out_specs=(vmem, vmem),
        scratch_shapes=[
            pltpu.VMEM((width_model, hidden_width), bf16),
            pltpu.VMEM((width_model, hidden_width), bf16),
            pltpu.VMEM((tp_count, hidden_width, half_width), bf16),
            pltpu.VMEM(w_out.shape, bf16),
            pltpu.VMEM((tp_count, seq_count, half_width), f32),
            pltpu.VMEM((tp_count, seq_count, half_width), f32),
            pltpu.VMEM((tp_count, seq_count, half_width), bf16),
            pltpu.VMEM((tp_count, seq_count, half_width), bf16),
            pltpu.VMEM((ep_count, cap, half_width), bf16),
            pltpu.VMEM((tp_count, ep_count, cap, half_width), bf16),
            pltpu.VMEM((ep_count, cap, hidden_width), bf16),
            pltpu.VMEM((n_parts, per_part, cap, half_width), bf16),
            pltpu.VMEM((n_parts, per_part, cap, half_width), bf16),
            pltpu.VMEM((n_parts, per_part, cap, half_width), bf16),
            pltpu.VMEM((ep_count, cap, half_width), bf16),
            pltpu.VMEM((ep_count, cap, half_width), bf16),
            dma((2,)),
            dma((ep_count,)),
            dma((ep_count,)),
            dma((ep_count,)),
            dma((ep_count,)),
            dma((n_parts,)),
            dma((n_parts,)),
            dma((ep_count,)),
            dma((ep_count,)),
            dma((5,)),
        ],
        compiler_params=pltpu.CompilerParams(
            collective_id=0, has_side_effects=True, vmem_limit_bytes=60 * 1024 * 1024
        ),
    )(
        mixed,
        w_out,
        tokens_in,
        norm_moe,
        router_group.T,
        router_expert.T,
        routes.T,
        expert_gate,
        expert_up,
        expert_down,
    )
    layer_out = (mid_half.astype(f32) + moe_out).astype(bf16)
    return (layer_out, state_out)


def solution(mesh):
    in_specs = (
        P("ep", None),
        P("ep", "tp", None, None),
        P(),
        P(None, "tp"),
        P(None, "tp"),
        P(None, "tp"),
        P(),
        P(None, "tp"),
        P("tp"),
        P(),
        P(None, "tp"),
        P("tp"),
        P("tp"),
        P("tp"),
        P("tp", None),
        P(),
        P(),
        P(),
        P("ep", None),
        P("ep", None, "tp"),
        P("ep", None, "tp"),
        P("ep", "tp", None),
    )
    out_specs = (P("ep", "tp"), P("ep", "tp", None, None))
    return jax.shard_map(shards, mesh=mesh, in_specs=in_specs, out_specs=out_specs, check_vma=False)
```
